32 devices in a mesh: sp: 8 (over z, x), tp: 4 (over y, core).
Axes of the slice: x: 2, y: 2, z: 4, core: 2. Of those that a mesh axis runs over, the one named last changes fastest.
Arguments:
- residual: bfloat16 [2048, 2048], P(('sp', 'tp')), may hold values from -6 to 6
- first_query: bfloat16 [2048, 512], P('sp', 'tp'), may hold values from -6 to 6
- second_query: bfloat16 [2048, 512], P('sp', 'tp'), may hold values from -6 to 6
- first_key: bfloat16 [2048, 512], P('sp', 'tp'), may hold values from -6 to 6
- second_key: bfloat16 [2048, 512], P('sp', 'tp'), may hold values from -6 to 6
- values: bfloat16 [2048, 1024], P('sp', 'tp'), may hold values from -6 to 6
- lambdas: float32 [8], P('tp'), may hold values from 0.3 to 0.8
- head_gain: float32 [128], replicated, may hold values from 0.1 to 1.9
- out_weight: bfloat16 [1024, 2048], P('tp'), may hold values from -0.1875 to 0.1875
- norm_gain: float32 [2048], replicated, may hold values from 0.1 to 1.9
- up_weight: bfloat16 [2048, 4096], P('sp', 'tp'), may hold values from -0.125 to 0.125
- down_weight: bfloat16 [4096, 2048], P('tp', 'sp'), may hold values from -0.09375 to 0.09375
Outputs:
- mixed: bfloat16 [2048, 2048], P(('sp', 'tp'))
The draws below stay inside these ranges and needn't reach their ends.
All inputs are finite; a program needn't handle non-finite values.
Results may differ from the reference program's by a relative error of at most 0.019.
Values may be sent and summed in bfloat16 or wider, within the bound.
A program may use at most 128 MiB of HBM per device.

```python
import jax
import jax.numpy as jnp
from jax import lax

D = 2048
HEADS = 8
HEAD = 64
VDIM = 128
FF = 4096
TOK_DEV = 256
TOKENS = 2048


def draw_entries(key, which_map, which_role):
    own_key = jax.random.fold_in(key, 100 * which_map + which_role)
    width = HEADS * HEAD
    data = jnp.clip(1.3 * jax.random.normal(own_key, (TOKENS, width), jnp.float32), -6.0, 6.0)
    return data.astype(jnp.bfloat16)


def draw_first_query(key, part):
    return draw_entries(key, 1, 0)


def draw_first_key(key, part):
    return draw_entries(key, 1, 1)


def draw_second_query(key, part):
    return draw_entries(key, 2, 0)


def draw_second_key(key, part):
    return draw_entries(key, 2, 1)


def steps_of(key, shape, split, least, top_value):
    level, own = 1.0, jax.random.fold_in(key, 6)
    for axis_at, blocks in split:
        heights = jnp.exp(jax.random.uniform(jax.random.fold_in(own, axis_at), (blocks,), jnp.float32, least / len(split), top_value / len(split)))
        level = level * jnp.repeat(heights, shape[axis_at] // blocks).reshape([-1 if axis == axis_at else 1 for axis in range(len(shape))])
    return level


def gaussian(key, dims, scale, most, shards=(), held_as=jnp.bfloat16):
    result = jax.random.normal(key, dims, jnp.float32) * scale
    if len(shards) > 0:
        result = steps_of(key, dims, shards, -0.22, 0.18) * result
    return jnp.clip(result, min=-most, max=most).astype(held_as)


def setup_inputs(seed: int = 0) -> dict:
    arg_keys = jax.random.split(jax.random.key(seed), 13)
    residual = gaussian(arg_keys[0], (TOKENS, D), 1.0, 6.0, ((0, 32),))
    first_query = draw_first_query(jax.random.fold_in(arg_keys[12], 71), 0)
    second_query = draw_second_query(jax.random.fold_in(arg_keys[12], 71), 0)
    first_key = draw_first_key(jax.random.fold_in(arg_keys[12], 71), 0)
    second_key = draw_second_key(jax.random.fold_in(arg_keys[12], 71), 0)
    values = gaussian(arg_keys[5], (TOKENS, HEADS * VDIM), 1.0, 6.0, ((0, 8), (1, 4)))
    lambdas = jnp.clip(0.3 + 0.5 * jax.random.uniform(arg_keys[6], (HEADS,), jnp.float32) ** steps_of(arg_keys[6], (HEADS,), ((0, 4),), -0.2, 0.2), 0.3, 0.8)
    head_gain = jnp.clip(1.0 + 0.18 * jax.random.normal(arg_keys[7], (VDIM,), jnp.float32), 0.1, 1.9)
    out_weight = gaussian(arg_keys[8], (HEADS * VDIM, D), (HEADS * VDIM) ** -0.5, 0.1875, ((0, 4),))
    norm_gain = jnp.clip(1.0 + 0.18 * jax.random.normal(arg_keys[9], (D,), jnp.float32), 0.1, 1.9)
    up_weight = gaussian(arg_keys[10], (D, FF), D ** -0.5, 0.125, ((0, 8), (1, 4)))
    down_weight = gaussian(arg_keys[11], (FF, D), FF ** -0.5, 0.09375, ((0, 4), (1, 8)))
    return dict(residual=residual, first_query=first_query, second_query=second_query, first_key=first_key, second_key=second_key, values=values, lambdas=lambdas, head_gain=head_gain, out_weight=out_weight, norm_gain=norm_gain, up_weight=up_weight, down_weight=down_weight)


def rotate(blocked, positions):
    half = blocked.shape[-1] // 2
    inverse = 10000.0 ** (-jnp.arange(0, half, dtype=jnp.float32) * 2.0 / blocked.shape[-1])
    angle = positions[:, None] * inverse[None, :]
    cosine = jnp.cos(angle)[:, None, :]
    sine = jnp.sin(angle)[:, None, :]
    first, second = (blocked[..., :half], blocked[..., half:])
    return jnp.concatenate([first * cosine - second * sine, second * cosine + first * sine], axis=-1)

def attend(queries, keys, vals):
    scores = jnp.dot(queries, keys.T, preferred_element_type=jnp.float32) * HEAD ** (-0.5)
    peak = lax.optimization_barrier(jnp.max(scores, axis=-1, keepdims=True))
    weights = jnp.exp(scores - peak)
    total = lax.optimization_barrier(jnp.sum(weights, axis=-1, keepdims=True))
    summed = jnp.dot(weights.astype(jnp.bfloat16), vals, preferred_element_type=jnp.float32)
    return summed / total

def layer_norm(stream, gain):
    center = stream - lax.optimization_barrier(jnp.mean(stream, axis=-1, keepdims=True))
    spread = lax.optimization_barrier(jnp.mean(center * center, axis=-1, keepdims=True))
    return center * lax.rsqrt(spread + 1e-05) * gain

def reference(residual, first_query, second_query, first_key, second_key, values, lambdas, head_gain, out_weight, norm_gain, up_weight, down_weight):
    length = residual.shape[0]
    positions = jnp.arange(length, dtype=jnp.float32)

    def prepare(source):
        turned = rotate(source.astype(jnp.float32).reshape(length, HEADS, HEAD), positions)
        return turned.astype(jnp.bfloat16).transpose(1, 0, 2)
    query_a, query_b = (prepare(first_query), prepare(second_query))
    key_a, key_b = (prepare(first_key), prepare(second_key))
    vals = values.reshape(length, HEADS, VDIM).transpose(1, 0, 2)

    def one_head(item):
        part_a, part_b, keys_a, keys_b, head_vals, weight = item

        def one_block(pair):
            return attend(pair[0], keys_a, head_vals) - weight * attend(pair[1], keys_b, head_vals)
        blocks = lax.map(one_block, (part_a.reshape(-1, TOK_DEV, HEAD), part_b.reshape(-1, TOK_DEV, HEAD)))
        return blocks.reshape(length, VDIM)
    diff = lax.map(one_head, (query_a, query_b, key_a, key_b, vals, lambdas))
    scale = lax.rsqrt(lax.optimization_barrier(jnp.mean(diff * diff, axis=-1, keepdims=True)) + 1e-05)
    heads_out = (diff * scale * head_gain * 0.8).astype(jnp.bfloat16)
    flat = heads_out.transpose(1, 0, 2).reshape(length, HEADS * VDIM)
    projected = jnp.dot(flat, out_weight, preferred_element_type=jnp.float32)
    normed = layer_norm(residual.astype(jnp.float32) + projected, norm_gain).astype(jnp.bfloat16)
    lifted = jnp.dot(normed, up_weight, preferred_element_type=jnp.float32)
    hidden = jnp.square(jax.nn.relu(lifted)).astype(jnp.bfloat16)
    lowered = jnp.dot(hidden, down_weight, preferred_element_type=jnp.float32)
    return (normed.astype(jnp.float32) + lowered).astype(jnp.bfloat16)
```

```python
import functools

import jax
import jax.numpy as jnp
from jax import lax
from jax.experimental import pallas as pl
from jax.experimental.pallas import tpu as pltpu
from jax.sharding import PartitionSpec as P


def rotate(blocked, positions):
    half = blocked.shape[-1] // 2
    inverse = 10000.0 ** (-jnp.arange(0, half, dtype=jnp.float32) * 2.0 / blocked.shape[-1])
    angle = positions[:, None] * inverse[None, :]
    cosine = jnp.cos(angle)[:, None, :]
    sine = jnp.sin(angle)[:, None, :]
    first, second = (blocked[..., :half], blocked[..., half:])
    return jnp.concatenate(
        [first * cosine - second * sine, second * cosine + first * sine], axis=-1
    )


def absorb(state, queries, keys, vals, factor):
    top, total, summed = state
    scores = jnp.einsum("qhe,khe->qhk", queries, keys, preferred_element_type=jnp.float32) * factor
    peak = jnp.maximum(top, jnp.max(scores, axis=-1))
    shrink = jnp.exp(top - peak)
    weights = jnp.exp(scores - peak[..., None])
    total = total * shrink + jnp.sum(weights, axis=-1)
    summed = summed * shrink[..., None] + jnp.einsum(
        "qhk,khe->qhe", weights.astype(jnp.bfloat16), vals, preferred_element_type=jnp.float32
    )
    return (peak, total, summed)


def layer_norm(stream, gain):
    center = stream - jnp.mean(stream, axis=-1, keepdims=True)
    spread = jnp.mean(center * center, axis=-1, keepdims=True)
    return center * lax.rsqrt(spread + 1e-05) * gain


def local(
    residual,
    first_query,
    second_query,
    first_key,
    second_key,
    values,
    lambdas,
    head_gain,
    out_weight,
    norm_gain,
    up_weight,
    down_weight,
):
    local_rows = first_query.shape[0]
    head_count = lambdas.shape[0]
    head_width = first_query.shape[1] // head_count
    value_width = values.shape[1] // head_count
    quarter_rows = local_rows // lax.axis_size("tp")
    factor = head_width ** (-0.5)
    positions = (lax.axis_index("sp") * local_rows + jnp.arange(local_rows)).astype(jnp.float32)

    def prepare(source):
        turned = rotate(
            source.astype(jnp.float32).reshape(local_rows, head_count, head_width), positions
        )
        return turned.astype(jnp.bfloat16)

    query_a, query_b = (prepare(first_query), prepare(second_query))
    key_a = prepare(first_key).reshape(local_rows, head_count * head_width)
    key_b = prepare(second_key).reshape(local_rows, head_count * head_width)
    start_state = (
        jnp.full((local_rows, head_count), -1e30, jnp.float32),
        jnp.zeros((local_rows, head_count), jnp.float32),
        jnp.zeros((local_rows, head_count, value_width), jnp.float32),
    )
    piece_a = lax.all_gather(key_a, "sp", axis=0, tiled=True)
    piece_b = lax.all_gather(key_b, "sp", axis=0, tiled=True)
    piece_v = lax.all_gather(values, "sp", axis=0, tiled=True)
    count = piece_a.shape[0]
    block = 512
    blocks = count // block

    def advance(state, item):
        block_a, block_b, block_v = item
        return (
            (
                absorb(state[0], query_a, block_a, block_v, factor),
                absorb(state[1], query_b, block_b, block_v, factor),
            ),
            None,
        )

    items = (
        piece_a.reshape(blocks, block, head_count, head_width),
        piece_b.reshape(blocks, block, head_count, head_width),
        piece_v.reshape(blocks, block, head_count, value_width),
    )
    state_a, state_b = lax.scan(advance, (start_state, start_state), items)[0]
    diff = state_a[2] / state_a[1][..., None] - lambdas[None, :, None] * (
        state_b[2] / state_b[1][..., None]
    )
    scale = lax.rsqrt(jnp.mean(diff * diff, axis=-1, keepdims=True) + 1e-05)
    flat = (
        (diff * scale * head_gain * 0.8)
        .astype(jnp.bfloat16)
        .reshape(local_rows, head_count * value_width)
    )
    projected = lax.psum(
        jnp.dot(flat, out_weight, preferred_element_type=jnp.float32).astype(jnp.bfloat16), "tp"
    ).astype(jnp.float32)
    stream = lax.all_gather(residual, "tp", axis=0, tiled=True)
    whole = layer_norm(stream.astype(jnp.float32) + projected, norm_gain).astype(jnp.bfloat16)
    own_normed = lax.dynamic_slice_in_dim(
        whole, lax.axis_index("tp") * quarter_rows, quarter_rows, 0
    )
    lifted = jnp.dot(
        whole,
        lax.all_gather(up_weight, "sp", axis=0, tiled=True),
        preferred_element_type=jnp.float32,
    )
    down_full = lax.all_gather(down_weight, "sp", axis=1, tiled=True)
    hidden = jnp.square(jax.nn.relu(lifted)).astype(jnp.bfloat16)
    lowered = lax.psum_scatter(
        jnp.dot(hidden, down_full, preferred_element_type=jnp.float32).astype(jnp.bfloat16),
        "tp",
        scatter_dimension=0,
        tiled=True,
    ).astype(jnp.float32)
    return (own_normed.astype(jnp.float32) + lowered).astype(jnp.bfloat16)


BF = jnp.bfloat16
F32 = jnp.float32
VMEM_BUDGET = 40 * 2**20


def prep_kernel(heads, qa_ref, qb_ref, ka_ref, kb_ref, v_ref, cos_ref, sin_ref, qm_ref, kv_ref):
    rows, width = qa_ref.shape
    head_width = width // heads
    half = head_width // 2
    lane = lax.broadcasted_iota(jnp.int32, (rows, width), 1)
    low = (lane % head_width) < half
    cos, sin = cos_ref[...], sin_ref[...]

    def turn(ref):
        x = ref[...].astype(F32)
        other = jnp.where(low, pltpu.roll(x, width - half, 1), pltpu.roll(x, half, 1))
        return x * cos + other * sin

    for which, ref in enumerate((qa_ref, qb_ref)):
        q = turn(ref).astype(BF).astype(F32) * head_width ** (-0.5)
        for h in range(heads):
            own = (lane // head_width) == h
            qm_ref[which, h * rows : (h + 1) * rows, :] = jnp.where(own, q, 0.0).astype(BF)
    kv_ref[:, :width] = turn(ka_ref).astype(BF)
    kv_ref[:, width : 2 * width] = turn(kb_ref).astype(BF)
    kv_ref[:, 2 * width :] = v_ref[...]


def layer_kernel(
    n, nt, heads,
    qm, kv0, lam, hgain, ow0, res0, ngain, up0, dn0,
    out,
    kv, up, dn, ow, res, flat, normed, lifted, hidden, part, mine, got,
    top, total, summed, send, recv,
):
    s = lax.axis_index("sp")
    t = lax.axis_index("tp")
    rows, kv_width = kv0.shape
    width = qm.shape[2]
    value_width = (kv_width - 2 * width) // heads
    depth = up0.shape[0]
    units = up0.shape[1]
    model = ow0.shape[1]
    piece = res0.shape[0]
    mid = n // 2
    odd = s % 2
    place = (1 - odd) * (s // 2) + odd * (n - 1 - s // 2)

    def at_place(p):
        p = p % n
        hi = p // mid
        return (1 - hi) * (2 * p) + hi * (2 * (n - 1 - p) + 1)

    def owner(slot):
        return at_place(place - slot + n)

    right = {"sp": at_place(place + 1)}
    left = {"sp": at_place(place + n - 1)}
    mates = [{"tp": (t + d) % nt} for d in range(1, nt)]
    barrier = pltpu.get_barrier_semaphore()
    for peer in [right, left] + mates:
        pl.semaphore_signal(barrier, inc=1, device_id=peer, device_id_type=pl.DeviceIdType.MESH)
    pl.semaphore_wait(barrier, nt + 1)

    copies = []

    def remote(src, dst, peer):
        i = len(copies)
        c = pltpu.make_async_remote_copy(
            src_ref=src, dst_ref=dst, send_sem=send.at[i], recv_sem=recv.at[i],
            device_id=peer, device_id_type=pl.DeviceIdType.MESH,
        )
        c.start()
        copies.append(c)
        return c

    def ring(own, buf, k, lo=0, hi=None):
        size = own.shape[0]
        hi = size if hi is None else hi
        a, b = (lo, hi), (lo, hi)
        if k == mid:
            a, b = (0, size // 2), (size // 2, size)
        cut_a, cut_b = pl.ds(a[0], a[1] - a[0]), pl.ds(b[0], b[1] - b[0])
        src_a = own.at[cut_a] if k == 1 else buf.at[k - 1, cut_a]
        src_b = own.at[cut_b] if k == 1 else buf.at[n - k + 1, cut_b]
        return [
            remote(src_a, buf.at[k, cut_a], right),
            remote(src_b, buf.at[n - k, cut_b], left),
        ]

    def arrive(group):
        for c in group:
            c.wait_recv()

    def absorb(block):
        for which in range(2):
            keys = block[:, which * width : (which + 1) * width]
            for h in range(heads):
                at = which * heads + h
                scores = lax.dot_general(
                    keys, qm[which, h * rows : (h + 1) * rows, :],
                    (((1,), (1,)), ((), ())), preferred_element_type=F32,
                )
                old = top[at]
                peak = jnp.maximum(old, jnp.max(scores, axis=0, keepdims=True))
                shrink = jnp.exp(old - peak)
                e = jnp.exp(scores - peak)
                top[at] = peak
                total[at] = total[at] * shrink + jnp.sum(e, axis=0, keepdims=True)
                first = 2 * width + h * value_width
                vals = block[:, first : first + value_width]
                summed[at] = summed[at] * shrink + lax.dot_general(
                    vals, e.astype(BF), (((0,), (0,)), ((), ())), preferred_element_type=F32
                )

    def absorb_pair(k):
        def body(i, carry):
            absorb(kv[k + i * (n - 2 * k)])
            return carry

        lax.fori_loop(0, 2, body, 0)

    cuts = [(i * depth // mid, (i + 1) * depth // mid) for i in range(mid)]
    got_kv = ring(kv0, kv, 1)
    got_res = [remote(res0, res.at[t], m) for m in mates]
    got_ow = [remote(ow0, ow.at[d], m) for d, m in enumerate(mates)]
    got_up = ring(up0, up, 1, *cuts[0])
    top[...] = jnp.full(top.shape, -1e30, F32)
    total[...] = jnp.zeros(total.shape, F32)
    summed[...] = jnp.zeros(summed.shape, F32)
    res[t] = res0[...]
    absorb(kv0[...])
    for k in range(1, mid):
        arrive(got_kv)
        got_kv = ring(kv0, kv, k + 1)
        got_up += ring(up0, up, 1, *cuts[k])
        if k == mid - 1:
            got_dn = ring(dn0, dn, 1)
        absorb_pair(k)
    arrive(got_kv)
    absorb(kv[mid])

    for h in range(heads):
        a = summed[h] / total[h]
        b = summed[heads + h] / total[heads + h]
        diff = a - lam[h] * b
        scale = lax.rsqrt(jnp.mean(diff * diff, axis=0, keepdims=True) + 1e-05)
        done = diff * scale * hgain[...] * 0.8
        flat[0, :, h * value_width : (h + 1) * value_width] = done.T.astype(BF)

    arrive(got_up)
    got_up = ring(up0, up, 2)
    got_flat = [remote(flat.at[0], flat.at[d + 1], m) for d, m in enumerate(mates)]
    arrive(got_dn)
    got_dn = ring(dn0, dn, 2)
    arrive(got_res + got_ow + got_flat)

    chunk = piece
    def norm_rows(q, carry):
        rows_at = pl.ds(pl.multiple_of(q * chunk, chunk), chunk)
        stream = res[q].astype(F32) + jnp.dot(flat[0, rows_at, :], ow0[...], preferred_element_type=F32)
        for d in range(1, nt):
            stream += jnp.dot(flat[d, rows_at, :], ow[d - 1], preferred_element_type=F32)
        center = stream - jnp.mean(stream, axis=-1, keepdims=True)
        spread = jnp.mean(center * center, axis=-1, keepdims=True)
        row = (center * lax.rsqrt(spread + 1e-05) * ngain[...]).astype(BF)
        for i in range(n):
            normed[i, q] = row[:, i * depth : (i + 1) * depth]
        return carry

    lax.fori_loop(0, nt, norm_rows, 0)

    def lift(block, slot):
        x = normed[owner(slot)].reshape(rows, depth)
        return jnp.dot(x, block, preferred_element_type=F32)

    def lift_pair(k):
        def body(i, carry):
            slot = k + i * (n - 2 * k)
            lifted[...] += lift(up[slot], slot)
            return carry

        lax.fori_loop(0, 2, body, 0)

    lifted[...] = lift(up0[...], 0)
    lift_pair(1)
    for k in range(2, mid):
        arrive(got_up)
        got_up = ring(up0, up, k + 1)
        lift_pair(k)
        arrive(got_dn)
        got_dn = ring(dn0, dn, k + 1)
    arrive(got_up)
    h = jnp.maximum(lifted[...] + lift(up[mid], mid), 0.0)
    hidden[...] = (h * h).astype(BF)

    waits = []

    def lower(block, slot):
        y = jnp.dot(hidden[...], block, preferred_element_type=F32).reshape(nt, piece, depth)
        mine[slot] = y
        part[slot] = y.astype(BF)

    def share(slot):
        waits.append((slot, [
            remote(part.at[slot, (t + d) % nt], got.at[slot, d - 1], mates[d - 1])
            for d in range(1, nt)
        ]))

    def finish(slot, group):
        arrive(group)
        who = owner(slot)
        y = normed[who, t].astype(F32) + mine[slot, t]
        for d in range(nt - 1):
            y += got[slot, d].astype(F32)
        out[:, pl.ds(pl.multiple_of(who * depth, depth), depth)] = y.astype(BF)

    lower(dn0[...], 0)
    for k in range(1, mid):
        lower(dn[k], k)
        share(0 if k == 1 else n - k + 1)
        lower(dn[n - k], n - k)
        share(k)
    share(mid + 1)
    for slot, group in waits[:-2]:
        finish(slot, group)
    arrive(got_dn)
    lower(dn[mid], mid)
    for slot, group in waits[-2:]:
        finish(slot, group)
    share(mid)
    finish(*waits[-1])
    for c in copies:
        c.wait_send()


def fused(n, nt, residual, first_query, second_query, first_key, second_key, values,
          lambdas, head_gain, out_weight, norm_gain, up_weight, down_weight):
    rows, width = first_query.shape
    heads = lambdas.shape[0]
    head_width = width // heads
    value_width = values.shape[1] // heads
    half = head_width // 2
    depth, units = up_weight.shape
    model = out_weight.shape[1]
    piece = residual.shape[0]
    positions = (lax.axis_index("sp") * rows + jnp.arange(rows)).astype(F32)
    inverse = 10000.0 ** (-jnp.arange(0, half, dtype=F32) * 2.0 / head_width)
    angle = positions[:, None] * inverse[None, :]
    cosine, sine = jnp.cos(angle), jnp.sin(angle)
    cosine = jnp.concatenate([cosine] * (2 * heads), axis=1)
    sine = jnp.concatenate([-sine, sine] * heads, axis=1)
    kv_width = 2 * width + heads * value_width
    qm, kv0 = pl.pallas_call(
        functools.partial(prep_kernel, heads),
        out_shape=(
            jax.ShapeDtypeStruct((2, heads * rows, width), BF),
            jax.ShapeDtypeStruct((rows, kv_width), BF),
        ),
        name="prepare",
    )(first_query, second_query, first_key, second_key, values, cosine, sine)
    vmem = pl.BlockSpec(memory_space=pltpu.VMEM)
    smem = pl.BlockSpec(memory_space=pltpu.SMEM)
    mid = n // 2
    count = 2 * mid + 2 * (2 * mid - 1) + 2 * mid + 3 * (nt - 1) + n * (nt - 1)
    maps = 2 * heads
    return pl.pallas_call(
        functools.partial(layer_kernel, n, nt, heads),
        out_shape=jax.ShapeDtypeStruct((piece, model), BF),
        in_specs=[vmem, vmem, smem] + [vmem] * 6,
        out_specs=vmem,
        scratch_shapes=[
            pltpu.VMEM((n, rows, kv_width), BF),
            pltpu.VMEM((n, depth, units), BF),
            pltpu.VMEM((n, units, depth), BF),
            pltpu.VMEM((nt - 1,) + out_weight.shape, BF),
            pltpu.VMEM((nt, piece, model), BF),
            pltpu.VMEM((nt, rows, heads * value_width), BF),
            pltpu.VMEM((n, nt, piece, depth), BF),
            pltpu.VMEM((rows, units), F32),
            pltpu.VMEM((rows, units), BF),
            pltpu.VMEM((n, nt, piece, depth), BF),
            pltpu.VMEM((n, nt, piece, depth), F32),
            pltpu.VMEM((n, nt - 1, piece, depth), BF),
            pltpu.VMEM((maps, 1, rows), F32),
            pltpu.VMEM((maps, 1, rows), F32),
            pltpu.VMEM((maps, value_width, rows), F32),
            pltpu.SemaphoreType.DMA((count,)),
            pltpu.SemaphoreType.DMA((count,)),
        ],
        compiler_params=pltpu.CompilerParams(
            collective_id=0, has_side_effects=True, vmem_limit_bytes=60 * 2**20
        ),
        name="layer",
    )(qm, kv0, lambdas, head_gain.reshape(-1, 1), out_weight, residual,
      norm_gain.reshape(1, -1), up_weight, down_weight)


def choose(*args):
    n, nt = lax.axis_size("sp"), lax.axis_size("tp")
    gathered = n * sum(a.size * a.dtype.itemsize for a in (args[3], args[4], args[5], args[10], args[11]))
    gathered += nt * sum(a.size * a.dtype.itemsize for a in (args[0], args[8]))
    if n % 2 == 0 and n >= 6 and 2 * gathered <= VMEM_BUDGET:
        return fused(n, nt, *args)
    return local(*args)


def solution(mesh):
    in_specs = (
        P(("sp", "tp"), None),
        P("sp", "tp"),
        P("sp", "tp"),
        P("sp", "tp"),
        P("sp", "tp"),
        P("sp", "tp"),
        P("tp"),
        P(),
        P("tp", None),
        P(),
        P("sp", "tp"),
        P("tp", "sp"),
    )
    out_specs = P(("sp", "tp"), None)
    return jax.shard_map(choose, mesh=mesh, in_specs=in_specs, out_specs=out_specs, check_vma=False)
```

```python
import functools

import jax
import jax.numpy as jnp
from jax import lax
from jax.experimental import pallas as pl
from jax.experimental.pallas import tpu as pltpu
from jax.sharding import PartitionSpec as P


def rotate(blocked, positions):
    half = blocked.shape[-1] // 2
    inverse = 10000.0 ** (-jnp.arange(0, half, dtype=jnp.float32) * 2.0 / blocked.shape[-1])
    angle = positions[:, None] * inverse[None, :]
    cosine = jnp.cos(angle)[:, None, :]
    sine = jnp.sin(angle)[:, None, :]
    first, second = (blocked[..., :half], blocked[..., half:])
    return jnp.concatenate(
        [first * cosine - second * sine, second * cosine + first * sine], axis=-1
    )


def absorb(state, queries, keys, vals, factor):
    top, total, summed = state
    scores = jnp.einsum("qhe,khe->qhk", queries, keys, preferred_element_type=jnp.float32) * factor
    peak = jnp.maximum(top, jnp.max(scores, axis=-1))
    shrink = jnp.exp(top - peak)
    weights = jnp.exp(scores - peak[..., None])
    total = total * shrink + jnp.sum(weights, axis=-1)
    summed = summed * shrink[..., None] + jnp.einsum(
        "qhk,khe->qhe", weights.astype(jnp.bfloat16), vals, preferred_element_type=jnp.float32
    )
    return (peak, total, summed)


def layer_norm(stream, gain):
    center = stream - jnp.mean(stream, axis=-1, keepdims=True)
    spread = jnp.mean(center * center, axis=-1, keepdims=True)
    return center * lax.rsqrt(spread + 1e-05) * gain


def local(
    residual,
    first_query,
    second_query,
    first_key,
    second_key,
    values,
    lambdas,
    head_gain,
    out_weight,
    norm_gain,
    up_weight,
    down_weight,
):
    local_rows = first_query.shape[0]
    head_count = lambdas.shape[0]
    head_width = first_query.shape[1] // head_count
    value_width = values.shape[1] // head_count
    quarter_rows = local_rows // lax.axis_size("tp")
    factor = head_width ** (-0.5)
    positions = (lax.axis_index("sp") * local_rows + jnp.arange(local_rows)).astype(jnp.float32)

    def prepare(source):
        turned = rotate(
            source.astype(jnp.float32).reshape(local_rows, head_count, head_width), positions
        )
        return turned.astype(jnp.bfloat16)

    query_a, query_b = (prepare(first_query), prepare(second_query))
    key_a = prepare(first_key).reshape(local_rows, head_count * head_width)
    key_b = prepare(second_key).reshape(local_rows, head_count * head_width)
    start_state = (
        jnp.full((local_rows, head_count), -1e30, jnp.float32),
        jnp.zeros((local_rows, head_count), jnp.float32),
        jnp.zeros((local_rows, head_count, value_width), jnp.float32),
    )
    piece_a = lax.all_gather(key_a, "sp", axis=0, tiled=True)
    piece_b = lax.all_gather(key_b, "sp", axis=0, tiled=True)
    piece_v = lax.all_gather(values, "sp", axis=0, tiled=True)
    count = piece_a.shape[0]
    block = 512
    blocks = count // block

    def advance(state, item):
        block_a, block_b, block_v = item
        return (
            (
                absorb(state[0], query_a, block_a, block_v, factor),
                absorb(state[1], query_b, block_b, block_v, factor),
            ),
            None,
        )

    items = (
        piece_a.reshape(blocks, block, head_count, head_width),
        piece_b.reshape(blocks, block, head_count, head_width),
        piece_v.reshape(blocks, block, head_count, value_width),
    )
    state_a, state_b = lax.scan(advance, (start_state, start_state), items)[0]
    diff = state_a[2] / state_a[1][..., None] - lambdas[None, :, None] * (
        state_b[2] / state_b[1][..., None]
    )
    scale = lax.rsqrt(jnp.mean(diff * diff, axis=-1, keepdims=True) + 1e-05)
    flat = (
        (diff * scale * head_gain * 0.8)
        .astype(jnp.bfloat16)
        .reshape(local_rows, head_count * value_width)
    )
    projected = lax.psum(
        jnp.dot(flat, out_weight, preferred_element_type=jnp.float32).astype(jnp.bfloat16), "tp"
    ).astype(jnp.float32)
    stream = lax.all_gather(residual, "tp", axis=0, tiled=True)
    whole = layer_norm(stream.astype(jnp.float32) + projected, norm_gain).astype(jnp.bfloat16)
    own_normed = lax.dynamic_slice_in_dim(
        whole, lax.axis_index("tp") * quarter_rows, quarter_rows, 0
    )
    lifted = jnp.dot(
        whole,
        lax.all_gather(up_weight, "sp", axis=0, tiled=True),
        preferred_element_type=jnp.float32,
    )
    down_full = lax.all_gather(down_weight, "sp", axis=1, tiled=True)
    hidden = jnp.square(jax.nn.relu(lifted)).astype(jnp.bfloat16)
    lowered = lax.psum_scatter(
        jnp.dot(hidden, down_full, preferred_element_type=jnp.float32).astype(jnp.bfloat16),
        "tp",
        scatter_dimension=0,
        tiled=True,
    ).astype(jnp.float32)
    return (own_normed.astype(jnp.float32) + lowered).astype(jnp.bfloat16)


BF = jnp.bfloat16
F32 = jnp.float32
VMEM_BUDGET = 40 * 2**20


def layer_kernel(
    n, nt, heads,
    qa, qb, ka, kb, v0, inverse, lam, hgain, ow0, res0, ngain, up0, dn0,
    out,
    qm, kv0, kv, up, dn, ow, res, flat, normed, lifted, hidden, part, mine, got,
    top, total, summed, send, recv,
):
    s = lax.axis_index("sp")
    t = lax.axis_index("tp")
    rows, kv_width = kv0.shape
    width = qm.shape[2]
    value_width = (kv_width - 2 * width) // heads
    depth = up0.shape[0]
    units = up0.shape[1]
    model = ow0.shape[1]
    piece = res0.shape[0]
    mid = n // 2
    odd = s % 2
    place = (1 - odd) * (s // 2) + odd * (n - 1 - s // 2)

    def at_place(p):
        p = p % n
        hi = p // mid
        return (1 - hi) * (2 * p) + hi * (2 * (n - 1 - p) + 1)

    def owner(slot):
        return at_place(place - slot + n)

    right = {"sp": at_place(place + 1)}
    left = {"sp": at_place(place + n - 1)}
    mates = [{"tp": (t + d) % nt} for d in range(1, nt)]
    barrier = pltpu.get_barrier_semaphore()
    for peer in [right, left] + mates:
        pl.semaphore_signal(barrier, inc=1, device_id=peer, device_id_type=pl.DeviceIdType.MESH)
    pl.semaphore_wait(barrier, nt + 1)

    copies = []

    def remote(src, dst, peer):
        i = len(copies)
        c = pltpu.make_async_remote_copy(
            src_ref=src, dst_ref=dst, send_sem=send.at[i], recv_sem=recv.at[i],
            device_id=peer, device_id_type=pl.DeviceIdType.MESH,
        )
        c.start()
        copies.append(c)
        return c

    own_of = {"kv": (kv0, kv), "up": (up0, up), "dn": (dn0, dn)}
    groups = {}

    def issue(name, k, *which):
        own, buf = own_of[name]
        size = own.shape[0]
        for i in which:
            if k > 1:
                ready(name, k - 1, i)
            a = pl.ds(i * (size // 2), size // 2)
            b = pl.ds((1 - i) * (size // 2), size // 2)
            src_a = own.at[a] if k == 1 else buf.at[k - 1, a]
            src_b = own.at[b] if k == 1 else buf.at[n - k + 1, b]
            groups[name, k, i] = [
                remote(src_a, buf.at[k, a], right),
                remote(src_b, buf.at[n - k, b], left),
            ]

    def ready(name, k, *which):
        for i in which:
            arrive(groups[name, k, i])
            groups[name, k, i] = []

    def arrive(group):
        for c in group:
            c.wait_recv()

    def absorb(block):
        for which in range(2):
            keys = block[:, which * width : (which + 1) * width]
            for h in range(heads):
                at = which * heads + h
                scores = lax.dot_general(
                    keys, qm[which, h * rows : (h + 1) * rows, :],
                    (((1,), (1,)), ((), ())), preferred_element_type=F32,
                )
                old = top[at]
                peak = jnp.maximum(old, jnp.max(scores, axis=0, keepdims=True))
                shrink = jnp.exp(old - peak)
                e = jnp.exp(scores - peak)
                top[at] = peak
                total[at] = total[at] * shrink + jnp.sum(e, axis=0, keepdims=True)
                first = 2 * width + h * value_width
                vals = block[:, first : first + value_width]
                summed[at] = summed[at] * shrink + lax.dot_general(
                    vals, e.astype(BF), (((0,), (0,)), ((), ())), preferred_element_type=F32
                )

    def absorb_pair(k):
        def body(i, carry):
            absorb(kv[k + i * (n - 2 * k)])
            return carry

        lax.fori_loop(0, 2, body, 0)

    partner = {"tp": t + 1 - 2 * (t % 2)}
    issue("up", 1, 0)
    across = range(2, nt, 2)
    far = [
        (d, [remote(res0, res.at[t], {"tp": (t + d) % nt}), remote(ow0, ow.at[t], {"tp": (t + d) % nt})])
        for d in across
    ]
    near = [remote(res0, res.at[t], partner), remote(ow0, ow.at[t], partner)]
    head_width = width // heads
    half = head_width // 2
    lane = lax.broadcasted_iota(jnp.int32, (rows, width), 1)
    low = (lane % head_width) < half
    position = (lax.broadcasted_iota(jnp.int32, (rows, width), 0) + s * rows).astype(F32)
    angle = position * inverse[...]
    cos = jnp.cos(angle)
    sin = jnp.sin(angle)
    sin = jnp.where(low, -sin, sin)

    def turn(ref):
        x = ref[...].astype(F32)
        other = jnp.where(low, pltpu.roll(x, width - half, 1), pltpu.roll(x, half, 1))
        return x * cos + other * sin

    kv0[:, 2 * width :] = v0[...]
    kv0[:, :width] = turn(ka).astype(BF)
    kv0[:, width : 2 * width] = turn(kb).astype(BF)
    for which, ref in enumerate((qa, qb)):
        q = turn(ref).astype(BF).astype(F32) * head_width ** (-0.5)
        for h in range(heads):
            own = (lane // head_width) == h
            qm[which, h * rows : (h + 1) * rows, :] = jnp.where(own, q, 0.0).astype(BF)
    issue("kv", 1, 0, 1)
    issue("up", 1, 1)
    top[...] = jnp.full(top.shape, -1e30, F32)
    total[...] = jnp.zeros(total.shape, F32)
    summed[...] = jnp.zeros(summed.shape, F32)
    res[t] = res0[...]
    absorb(kv0[...])
    fillers = [("dn", 1, 0), ("dn", 1, 1), ("up", 2, 0, 1)]
    for k in range(1, mid):
        issue("kv", k + 1, 0)
        ready("kv", k, 1)
        if k + 1 < mid:
            issue("kv", k + 1, 1)
        if fillers:
            issue(*fillers.pop(0))
        absorb_pair(k)
    for filler in fillers:
        issue(*filler)
    ready("kv", mid, 0)
    absorb(kv[mid])

    for h in range(heads):
        a = summed[h] / total[h]
        b = summed[heads + h] / total[heads + h]
        diff = a - lam[h] * b
        scale = lax.rsqrt(jnp.mean(diff * diff, axis=0, keepdims=True) + 1e-05)
        done = (diff * scale).T * hgain[...] * 0.8
        flat[0, :, h * value_width : (h + 1) * value_width] = done.astype(BF)

    got_flat = [remote(flat.at[0], flat.at[d + 1], m) for d, m in enumerate(mates)]
    issue("dn", 2, 0, 1)
    for d, pair in far:
        arrive(pair)
        there = (t + nt - d) % nt
        near += [remote(res.at[there], res.at[there], partner), remote(ow.at[there], ow.at[there], partner)]
    arrive(near + got_flat)

    chunk = piece
    def norm_rows(q, carry):
        rows_at = pl.ds(pl.multiple_of(q * chunk, chunk), chunk)
        stream = res[q].astype(F32) + jnp.dot(flat[0, rows_at, :], ow0[...], preferred_element_type=F32)
        for d in range(1, nt):
            stream += jnp.dot(flat[d, rows_at, :], ow[(t + nt - d) % nt], preferred_element_type=F32)
        center = stream - jnp.mean(stream, axis=-1, keepdims=True)
        spread = jnp.mean(center * center, axis=-1, keepdims=True)
        row = (center * lax.rsqrt(spread + 1e-05) * ngain[...]).astype(BF)
        for i in range(n):
            normed[i, q] = row[:, i * depth : (i + 1) * depth]
        return carry

    lax.fori_loop(0, nt, norm_rows, 0)

    def lift(block, slot):
        x = normed[owner(slot)].reshape(rows, depth)
        return jnp.dot(x, block, preferred_element_type=F32)

    def lift_pair(k):
        def body(i, carry):
            slot = k + i * (n - 2 * k)
            lifted[...] += lift(up[slot], slot)
            return carry

        lax.fori_loop(0, 2, body, 0)

    lifted[...] = lift(up0[...], 0)
    ready("up", 1, 0, 1)
    lift_pair(1)
    for k in range(2, mid):
        issue("up", k + 1, 0)
        if k + 1 < mid:
            issue("up", k + 1, 1)
        if k > 2:
            issue("dn", k, 0, 1)
        ready("up", k, 1)
        lift_pair(k)
    ready("up", mid, 0)
    h = jnp.maximum(lifted[...] + lift(up[mid], mid), 0.0)
    hidden[...] = (h * h).astype(BF)

    waits = []

    def lower(block, slot):
        y = jnp.dot(hidden[...], block, preferred_element_type=F32).reshape(nt, piece, depth)
        mine[slot] = y
        part[slot] = y.astype(BF)

    def share(slot):
        waits.append((slot, [
            remote(part.at[slot, (t + d) % nt], got.at[slot, d - 1], mates[d - 1])
            for d in range(1, nt)
        ]))

    def finish(slot, group):
        arrive(group)
        who = owner(slot)
        y = normed[who, t].astype(F32) + mine[slot, t]
        for d in range(nt - 1):
            y += got[slot, d].astype(F32)
        out[:, pl.ds(pl.multiple_of(who * depth, depth), depth)] = y.astype(BF)

    lower(dn0[...], 0)
    ready("dn", 1, 0, 1)
    last = 0
    for k in range(1, mid):
        if k == mid - 1:
            issue("dn", mid, 0)
        ready("dn", k, 0, 1)
        for slot in (k, n - k):
            lower(dn[slot], slot)
            share(last)
            last = slot
    share(last)
    for slot, group in waits[:-2]:
        finish(slot, group)
    ready("dn", mid, 0)
    lower(dn[mid], mid)
    for slot, group in waits[-2:]:
        finish(slot, group)
    share(mid)
    finish(*waits[-1])
    for c in copies:
        c.wait_send()


def fused(n, nt, residual, first_query, second_query, first_key, second_key, values,
          lambdas, head_gain, out_weight, norm_gain, up_weight, down_weight):
    rows, width = first_query.shape
    heads = lambdas.shape[0]
    head_width = width // heads
    value_width = values.shape[1] // heads
    half = head_width // 2
    depth, units = up_weight.shape
    model = out_weight.shape[1]
    piece = residual.shape[0]
    inverse = 10000.0 ** (-jnp.arange(0, half, dtype=F32) * 2.0 / head_width)
    inverse = jnp.concatenate([inverse] * (2 * heads))[None, :]
    kv_width = 2 * width + heads * value_width
    vmem = pl.BlockSpec(memory_space=pltpu.VMEM)
    smem = pl.BlockSpec(memory_space=pltpu.SMEM)
    mid = n // 2
    count = 6 * (n - 1) + 3 * nt + (n + 1) * (nt - 1)
    maps = 2 * heads
    return pl.pallas_call(
        functools.partial(layer_kernel, n, nt, heads),
        out_shape=jax.ShapeDtypeStruct((piece, model), BF),
        in_specs=[vmem] * 6 + [smem] + [vmem] * 6,
        out_specs=vmem,
        scratch_shapes=[
            pltpu.VMEM((2, heads * rows, width), BF),
            pltpu.VMEM((rows, kv_width), BF),
            pltpu.VMEM((n, rows, kv_width), BF),
            pltpu.VMEM((n, depth, units), BF),
            pltpu.VMEM((n, units, depth), BF),
            pltpu.VMEM((nt,) + out_weight.shape, BF),
            pltpu.VMEM((nt, piece, model), BF),
            pltpu.VMEM((nt, rows, heads * value_width), BF),
            pltpu.VMEM((n, nt, piece, depth), BF),
            pltpu.VMEM((rows, units), F32),
            pltpu.VMEM((rows, units), BF),
            pltpu.VMEM((n, nt, piece, depth), BF),
            pltpu.VMEM((n, nt, piece, depth), F32),
            pltpu.VMEM((n, nt - 1, piece, depth), BF),
            pltpu.VMEM((maps, 1, rows), F32),
            pltpu.VMEM((maps, 1, rows), F32),
            pltpu.VMEM((maps, value_width, rows), F32),
            pltpu.SemaphoreType.DMA((count,)),
            pltpu.SemaphoreType.DMA((count,)),
        ],
        compiler_params=pltpu.CompilerParams(
            collective_id=0, has_side_effects=True, vmem_limit_bytes=60 * 2**20
        ),
        name="layer",
    )(first_query, second_query, first_key, second_key, values, inverse,
      lambdas, head_gain.reshape(1, -1), out_weight, residual,
      norm_gain.reshape(1, -1), up_weight, down_weight)


def choose(*args):
    n, nt = lax.axis_size("sp"), lax.axis_size("tp")
    gathered = n * sum(a.size * a.dtype.itemsize for a in (args[3], args[4], args[5], args[10], args[11]))
    gathered += nt * sum(a.size * a.dtype.itemsize for a in (args[0], args[8]))
    if n % 2 == 0 and n >= 6 and nt % 2 == 0 and 2 * gathered <= VMEM_BUDGET:
        return fused(n, nt, *args)
    return local(*args)


def solution(mesh):
    in_specs = (
        P(("sp", "tp"), None),
        P("sp", "tp"),
        P("sp", "tp"),
        P("sp", "tp"),
        P("sp", "tp"),
        P("sp", "tp"),
        P("tp"),
        P(),
        P("tp", None),
        P(),
        P("sp", "tp"),
        P("tp", "sp"),
    )
    out_specs = P(("sp", "tp"), None)
    return jax.shard_map(choose, mesh=mesh, in_specs=in_specs, out_specs=out_specs, check_vma=False)
```

```python
import functools

import jax
import jax.numpy as jnp
import numpy as np
from jax import lax
from jax.experimental import pallas as pl
from jax.experimental.pallas import tpu as pltpu
from jax.sharding import PartitionSpec as P


def rotate(blocked, positions):
    half = blocked.shape[-1] // 2
    inverse = 10000.0 ** (-jnp.arange(0, half, dtype=jnp.float32) * 2.0 / blocked.shape[-1])
    angle = positions[:, None] * inverse[None, :]
    cosine = jnp.cos(angle)[:, None, :]
    sine = jnp.sin(angle)[:, None, :]
    first, second = (blocked[..., :half], blocked[..., half:])
    return jnp.concatenate(
        [first * cosine - second * sine, second * cosine + first * sine], axis=-1
    )


def absorb(state, queries, keys, vals, factor):
    top, total, summed = state
    scores = jnp.einsum("qhe,khe->qhk", queries, keys, preferred_element_type=jnp.float32) * factor
    peak = jnp.maximum(top, jnp.max(scores, axis=-1))
    shrink = jnp.exp(top - peak)
    weights = jnp.exp(scores - peak[..., None])
    total = total * shrink + jnp.sum(weights, axis=-1)
    summed = summed * shrink[..., None] + jnp.einsum(
        "qhk,khe->qhe", weights.astype(jnp.bfloat16), vals, preferred_element_type=jnp.float32
    )
    return (peak, total, summed)


def layer_norm(stream, gain):
    center = stream - jnp.mean(stream, axis=-1, keepdims=True)
    spread = jnp.mean(center * center, axis=-1, keepdims=True)
    return center * lax.rsqrt(spread + 1e-05) * gain


def local(
    residual,
    first_query,
    second_query,
    first_key,
    second_key,
    values,
    lambdas,
    head_gain,
    out_weight,
    norm_gain,
    up_weight,
    down_weight,
):
    local_rows = first_query.shape[0]
    head_count = lambdas.shape[0]
    head_width = first_query.shape[1] // head_count
    value_width = values.shape[1] // head_count
    quarter_rows = local_rows // lax.axis_size("tp")
    factor = head_width ** (-0.5)
    positions = (lax.axis_index("sp") * local_rows + jnp.arange(local_rows)).astype(jnp.float32)

    def prepare(source):
        turned = rotate(
            source.astype(jnp.float32).reshape(local_rows, head_count, head_width), positions
        )
        return turned.astype(jnp.bfloat16)

    query_a, query_b = (prepare(first_query), prepare(second_query))
    key_a = prepare(first_key).reshape(local_rows, head_count * head_width)
    key_b = prepare(second_key).reshape(local_rows, head_count * head_width)
    start_state = (
        jnp.full((local_rows, head_count), -1e30, jnp.float32),
        jnp.zeros((local_rows, head_count), jnp.float32),
        jnp.zeros((local_rows, head_count, value_width), jnp.float32),
    )
    piece_a = lax.all_gather(key_a, "sp", axis=0, tiled=True)
    piece_b = lax.all_gather(key_b, "sp", axis=0, tiled=True)
    piece_v = lax.all_gather(values, "sp", axis=0, tiled=True)
    count = piece_a.shape[0]
    block = 512
    blocks = count // block

    def advance(state, item):
        block_a, block_b, block_v = item
        return (
            (
                absorb(state[0], query_a, block_a, block_v, factor),
                absorb(state[1], query_b, block_b, block_v, factor),
            ),
            None,
        )

    items = (
        piece_a.reshape(blocks, block, head_count, head_width),
        piece_b.reshape(blocks, block, head_count, head_width),
        piece_v.reshape(blocks, block, head_count, value_width),
    )
    state_a, state_b = lax.scan(advance, (start_state, start_state), items)[0]
    diff = state_a[2] / state_a[1][..., None] - lambdas[None, :, None] * (
        state_b[2] / state_b[1][..., None]
    )
    scale = lax.rsqrt(jnp.mean(diff * diff, axis=-1, keepdims=True) + 1e-05)
    flat = (
        (diff * scale * head_gain * 0.8)
        .astype(jnp.bfloat16)
        .reshape(local_rows, head_count * value_width)
    )
    projected = lax.psum(
        jnp.dot(flat, out_weight, preferred_element_type=jnp.float32).astype(jnp.bfloat16), "tp"
    ).astype(jnp.float32)
    stream = lax.all_gather(residual, "tp", axis=0, tiled=True)
    whole = layer_norm(stream.astype(jnp.float32) + projected, norm_gain).astype(jnp.bfloat16)
    own_normed = lax.dynamic_slice_in_dim(
        whole, lax.axis_index("tp") * quarter_rows, quarter_rows, 0
    )
    lifted = jnp.dot(
        whole,
        lax.all_gather(up_weight, "sp", axis=0, tiled=True),
        preferred_element_type=jnp.float32,
    )
    down_full = lax.all_gather(down_weight, "sp", axis=1, tiled=True)
    hidden = jnp.square(jax.nn.relu(lifted)).astype(jnp.bfloat16)
    lowered = lax.psum_scatter(
        jnp.dot(hidden, down_full, preferred_element_type=jnp.float32).astype(jnp.bfloat16),
        "tp",
        scatter_dimension=0,
        tiled=True,
    ).astype(jnp.float32)
    return (own_normed.astype(jnp.float32) + lowered).astype(jnp.bfloat16)


BF = jnp.bfloat16
F32 = jnp.float32
VMEM_BUDGET = 40 * 2**20


def layer_kernel(
    n, nt, heads,
    qa, qb, ka, kb, v0, inverse, lam, hgain, ow0, res0, ngain, up0, dn0,
    out,
    qm, kv0, kv, up, dn, ow, res, flat, normed, lifted, hidden, part, mine, got,
    top, total, summed, send, recv, load,
):
    s = lax.axis_index("sp")
    t = lax.axis_index("tp")
    rows, kv_width = kv0.shape
    width = qm.shape[2]
    value_width = (kv_width - 2 * width) // heads
    depth = up0.shape[0]
    units = up0.shape[1]
    model = ow0.shape[1]
    piece = res0.shape[0]
    mid = n // 2
    odd = s % 2
    place = (1 - odd) * (s // 2) + odd * (n - 1 - s // 2)

    def at_place(p):
        p = p % n
        hi = p // mid
        return (1 - hi) * (2 * p) + hi * (2 * (n - 1 - p) + 1)

    def owner(slot):
        return at_place(place - slot + n)

    right = {"sp": at_place(place + 1)}
    left = {"sp": at_place(place + n - 1)}
    mates = [{"tp": (t + d) % nt} for d in range(1, nt)]
    loads = [
        pltpu.make_async_copy(src, dst, load.at[i])
        for i, (src, dst) in enumerate(((up0, up.at[0]), (dn0, dn.at[0]), (ow0, ow.at[t])))
    ]
    for c in loads:
        c.start()
    barrier = pltpu.get_barrier_semaphore()
    for peer in [right, left] + mates:
        pl.semaphore_signal(barrier, inc=1, device_id=peer, device_id_type=pl.DeviceIdType.MESH)
    pl.semaphore_wait(barrier, nt + 1)

    copies = []

    def remote(src, dst, peer):
        i = len(copies)
        c = pltpu.make_async_remote_copy(
            src_ref=src, dst_ref=dst, send_sem=send.at[i], recv_sem=recv.at[i],
            device_id=peer, device_id_type=pl.DeviceIdType.MESH,
        )
        c.start()
        copies.append(c)
        return c

    own_of = {"kv": (kv0, kv), "up": (up0, up), "dn": (dn0, dn)}
    groups = {}

    def issue(name, k, *which):
        own, buf = own_of[name]
        size = own.shape[0]
        for i in which:
            if k > 1:
                ready(name, k - 1, i)
            a = pl.ds(i * (size // 2), size // 2)
            b = pl.ds((1 - i) * (size // 2), size // 2)
            src_a = own.at[a] if k == 1 else buf.at[k - 1, a]
            src_b = own.at[b] if k == 1 else buf.at[n - k + 1, b]
            groups[name, k, i] = [
                remote(src_a, buf.at[k, a], right),
                remote(src_b, buf.at[n - k, b], left),
            ]

    def ready(name, k, *which):
        for i in which:
            arrive(groups[name, k, i])
            groups[name, k, i] = []

    def arrive(group):
        for c in group:
            c.wait_recv()

    def absorb(block):
        for which in range(2):
            keys = block[:, which * width : (which + 1) * width]
            for h in range(heads):
                at = which * heads + h
                scores = lax.dot_general(
                    keys, qm[which, h * rows : (h + 1) * rows, :],
                    (((1,), (1,)), ((), ())), preferred_element_type=F32,
                )
                old = top[at]
                peak = jnp.maximum(old, jnp.max(scores, axis=0, keepdims=True))
                shrink = jnp.exp(old - peak)
                e = jnp.exp(scores - peak)
                top[at] = peak
                total[at] = total[at] * shrink + jnp.sum(e, axis=0, keepdims=True)
                first = 2 * width + h * value_width
                vals = block[:, first : first + value_width]
                summed[at] = summed[at] * shrink + lax.dot_general(
                    vals, e.astype(BF), (((0,), (0,)), ((), ())), preferred_element_type=F32
                )

    def absorb_pair(k):
        def body(i, carry):
            absorb(kv[k + i * (n - 2 * k)])
            return carry

        lax.fori_loop(0, 2, body, 0)

    partner = {"tp": t + 1 - 2 * (t % 2)}
    issue("up", 1, 0)
    across = range(2, nt, 2)
    far = [
        (d, [remote(res0, res.at[t], {"tp": (t + d) % nt}), remote(ow0, ow.at[t], {"tp": (t + d) % nt})])
        for d in across
    ]
    near = [remote(res0, res.at[t], partner), remote(ow0, ow.at[t], partner)]
    head_width = width // heads
    half = head_width // 2
    lane = lax.broadcasted_iota(jnp.int32, (rows, width), 1)
    low = (lane % head_width) < half
    position = (lax.broadcasted_iota(jnp.int32, (rows, width), 0) + s * rows).astype(F32)
    angle = position * inverse[...]
    cos = jnp.cos(angle)
    sin = jnp.sin(angle)
    sin = jnp.where(low, -sin, sin)

    def turn(ref):
        x = ref[...].astype(F32)
        other = jnp.where(low, pltpu.roll(x, width - half, 1), pltpu.roll(x, half, 1))
        return x * cos + other * sin

    kv0[:, 2 * width :] = v0[...]
    kv0[:, :width] = turn(ka).astype(BF)
    kv0[:, width : 2 * width] = turn(kb).astype(BF)
    for which, ref in enumerate((qa, qb)):
        q = turn(ref).astype(BF).astype(F32) * head_width ** (-0.5)
        for h in range(heads):
            own = (lane // head_width) == h
            qm[which, h * rows : (h + 1) * rows, :] = jnp.where(own, q, 0.0).astype(BF)
    issue("kv", 1, 0, 1)
    issue("up", 1, 1)
    top[...] = jnp.full(top.shape, -1e30, F32)
    total[...] = jnp.zeros(total.shape, F32)
    summed[...] = jnp.zeros(summed.shape, F32)
    res[t] = res0[...]
    absorb(kv0[...])
    fillers = [("dn", 1, 0), ("dn", 1, 1), ("up", 2, 0, 1)]
    for k in range(1, mid):
        issue("kv", k + 1, 0)
        ready("kv", k, 1)
        if k + 1 < mid:
            issue("kv", k + 1, 1)
        if fillers:
            issue(*fillers.pop(0))
        absorb_pair(k)
    for filler in fillers:
        issue(*filler)
    ready("kv", mid, 0)
    issue("dn", 2, 0, 1)
    absorb(kv[mid])

    for h in range(heads):
        a = summed[h] / total[h]
        b = summed[heads + h] / total[heads + h]
        diff = a - lam[h] * b
        scale = lax.rsqrt(jnp.mean(diff * diff, axis=0, keepdims=True) + 1e-05)
        done = (diff * scale).T * hgain[...] * 0.8
        flat[0, :, h * value_width : (h + 1) * value_width] = done.astype(BF)

    got_flat = [remote(flat.at[0], flat.at[d + 1], m) for d, m in enumerate(mates)]
    for d, pair in far:
        arrive(pair)
        there = (t + nt - d) % nt
        near += [remote(res.at[there], res.at[there], partner), remote(ow.at[there], ow.at[there], partner)]
    arrive(near + got_flat)
    for c in loads:
        c.wait()

    chunk = piece
    def norm_rows(q, carry):
        rows_at = pl.ds(pl.multiple_of(q * chunk, chunk), chunk)
        stream = res[q].astype(F32) + jnp.dot(flat[0, rows_at, :], ow[t], preferred_element_type=F32)
        for d in range(1, nt):
            stream += jnp.dot(flat[d, rows_at, :], ow[(t + nt - d) % nt], preferred_element_type=F32)
        center = stream - jnp.mean(stream, axis=-1, keepdims=True)
        spread = jnp.mean(center * center, axis=-1, keepdims=True)
        row = (center * lax.rsqrt(spread + 1e-05) * ngain[...]).astype(BF)
        for i in range(n):
            normed[i, q] = row[:, i * depth : (i + 1) * depth]
        return carry

    lax.fori_loop(0, nt, norm_rows, 0)

    def lift(block, slot):
        x = normed[owner(slot)].reshape(rows, depth)
        return jnp.dot(x, block, preferred_element_type=F32)

    def lift_pair(k):
        def body(i, carry):
            slot = k + i * (n - 2 * k)
            lifted[...] += lift(up[slot], slot)
            return carry

        lax.fori_loop(0, 2, body, 0)

    lifted[...] = lift(up[0], 0)
    ready("up", 1, 0, 1)
    lift_pair(1)
    for k in range(2, mid):
        issue("up", k + 1, 0)
        if k + 1 < mid:
            issue("up", k + 1, 1)
        if k > 2:
            issue("dn", k, 0, 1)
        ready("up", k, 1)
        lift_pair(k)
    ready("up", mid, 0)
    h = jnp.maximum(lifted[...] + lift(up[mid], mid), 0.0)
    hidden[...] = (h * h).astype(BF)

    waits = []

    def lower(block, slot):
        y = jnp.dot(hidden[...], block, preferred_element_type=F32).reshape(nt, piece, depth)
        mine[slot] = y
        part[slot] = y.astype(BF)

    def share(slot):
        waits.append((slot, [
            remote(part.at[slot, (t + d) % nt], got.at[slot, d - 1], mates[d - 1])
            for d in range(1, nt)
        ]))

    def finish(slot, group):
        arrive(group)
        who = owner(slot)
        y = normed[who, t].astype(F32) + mine[slot, t]
        for d in range(nt - 1):
            y += got[slot, d].astype(F32)
        out[:, pl.ds(pl.multiple_of(who * depth, depth), depth)] = y.astype(BF)

    lower(dn[0], 0)
    ready("dn", 1, 0, 1)
    last = 0
    for k in range(1, mid):
        if k == mid - 1:
            issue("dn", mid, 0)
        ready("dn", k, 0, 1)
        for slot in (k, n - k):
            lower(dn[slot], slot)
            share(last)
            last = slot
    share(last)
    for slot, group in waits[:-2]:
        finish(slot, group)
    ready("dn", mid, 0)
    lower(dn[mid], mid)
    for slot, group in waits[-2:]:
        finish(slot, group)
    share(mid)
    finish(*waits[-1])
    for c in copies:
        c.wait_send()


def fused(n, nt, residual, first_query, second_query, first_key, second_key, values,
          lambdas, head_gain, out_weight, norm_gain, up_weight, down_weight):
    rows, width = first_query.shape
    heads = lambdas.shape[0]
    head_width = width // heads
    value_width = values.shape[1] // heads
    half = head_width // 2
    depth, units = up_weight.shape
    model = out_weight.shape[1]
    piece = residual.shape[0]
    inverse = 10000.0 ** (-np.arange(half) * 2.0 / head_width)
    inverse = np.tile(inverse, 2 * heads)[None, :].astype(np.float32)
    kv_width = 2 * width + heads * value_width
    vmem = pl.BlockSpec(memory_space=pltpu.VMEM)
    smem = pl.BlockSpec(memory_space=pltpu.SMEM)
    far = pl.BlockSpec(memory_space=pl.ANY)
    mid = n // 2
    count = 6 * (n - 1) + 3 * nt + (n + 1) * (nt - 1)
    maps = 2 * heads
    return pl.pallas_call(
        functools.partial(layer_kernel, n, nt, heads),
        out_shape=jax.ShapeDtypeStruct((piece, model), BF),
        in_specs=[vmem] * 6 + [smem, vmem, far, vmem, vmem, far, far],
        out_specs=vmem,
        scratch_shapes=[
            pltpu.VMEM((2, heads * rows, width), BF),
            pltpu.VMEM((rows, kv_width), BF),
            pltpu.VMEM((n, rows, kv_width), BF),
            pltpu.VMEM((n, depth, units), BF),
            pltpu.VMEM((n, units, depth), BF),
            pltpu.VMEM((nt,) + out_weight.shape, BF),
            pltpu.VMEM((nt, piece, model), BF),
            pltpu.VMEM((nt, rows, heads * value_width), BF),
            pltpu.VMEM((n, nt, piece, depth), BF),
            pltpu.VMEM((rows, units), F32),
            pltpu.VMEM((rows, units), BF),
            pltpu.VMEM((n, nt, piece, depth), BF),
            pltpu.VMEM((n, nt, piece, depth), F32),
            pltpu.VMEM((n, nt - 1, piece, depth), BF),
            pltpu.VMEM((maps, 1, rows), F32),
            pltpu.VMEM((maps, 1, rows), F32),
            pltpu.VMEM((maps, value_width, rows), F32),
            pltpu.SemaphoreType.DMA((count,)),
            pltpu.SemaphoreType.DMA((count,)),
            pltpu.SemaphoreType.DMA((3,)),
        ],
        compiler_params=pltpu.CompilerParams(
            collective_id=0, has_side_effects=True, vmem_limit_bytes=60 * 2**20
        ),
        name="layer",
    )(first_query, second_query, first_key, second_key, values, inverse,
      lambdas, head_gain.reshape(1, -1), out_weight, residual,
      norm_gain.reshape(1, -1), up_weight, down_weight)


def choose(*args):
    n, nt = lax.axis_size("sp"), lax.axis_size("tp")
    gathered = n * sum(a.size * a.dtype.itemsize for a in (args[3], args[4], args[5], args[10], args[11]))
    gathered += nt * sum(a.size * a.dtype.itemsize for a in (args[0], args[8]))
    if n % 2 == 0 and n >= 6 and nt % 2 == 0 and 2 * gathered <= VMEM_BUDGET:
        return fused(n, nt, *args)
    return local(*args)


def solution(mesh):
    in_specs = (
        P(("sp", "tp"), None),
        P("sp", "tp"),
        P("sp", "tp"),
        P("sp", "tp"),
        P("sp", "tp"),
        P("sp", "tp"),
        P("tp"),
        P(),
        P("tp", None),
        P(),
        P("sp", "tp"),
        P("tp", "sp"),
    )
    out_specs = P(("sp", "tp"), None)
    return jax.shard_map(choose, mesh=mesh, in_specs=in_specs, out_specs=out_specs, check_vma=False)
```

```python
import functools

import jax
import jax.numpy as jnp
import numpy as np
from jax import lax
from jax.experimental import pallas as pl
from jax.experimental.pallas import tpu as pltpu
from jax.sharding import PartitionSpec as P


def rotate(blocked, positions):
    half = blocked.shape[-1] // 2
    inverse = 10000.0 ** (-jnp.arange(0, half, dtype=jnp.float32) * 2.0 / blocked.shape[-1])
    angle = positions[:, None] * inverse[None, :]
    cosine = jnp.cos(angle)[:, None, :]
    sine = jnp.sin(angle)[:, None, :]
    first, second = (blocked[..., :half], blocked[..., half:])
    return jnp.concatenate(
        [first * cosine - second * sine, second * cosine + first * sine], axis=-1
    )


def absorb(state, queries, keys, vals, factor):
    top, total, summed = state
    scores = jnp.einsum("qhe,khe->qhk", queries, keys, preferred_element_type=jnp.float32) * factor
    peak = jnp.maximum(top, jnp.max(scores, axis=-1))
    shrink = jnp.exp(top - peak)
    weights = jnp.exp(scores - peak[..., None])
    total = total * shrink + jnp.sum(weights, axis=-1)
    summed = summed * shrink[..., None] + jnp.einsum(
        "qhk,khe->qhe", weights.astype(jnp.bfloat16), vals, preferred_element_type=jnp.float32
    )
    return (peak, total, summed)


def layer_norm(stream, gain):
    center = stream - jnp.mean(stream, axis=-1, keepdims=True)
    spread = jnp.mean(center * center, axis=-1, keepdims=True)
    return center * lax.rsqrt(spread + 1e-05) * gain


def local(
    residual,
    first_query,
    second_query,
    first_key,
    second_key,
    values,
    lambdas,
    head_gain,
    out_weight,
    norm_gain,
    up_weight,
    down_weight,
):
    local_rows = first_query.shape[0]
    head_count = lambdas.shape[0]
    head_width = first_query.shape[1] // head_count
    value_width = values.shape[1] // head_count
    quarter_rows = local_rows // lax.axis_size("tp")
    factor = head_width ** (-0.5)
    positions = (lax.axis_index("sp") * local_rows + jnp.arange(local_rows)).astype(jnp.float32)

    def prepare(source):
        turned = rotate(
            source.astype(jnp.float32).reshape(local_rows, head_count, head_width), positions
        )
        return turned.astype(jnp.bfloat16)

    query_a, query_b = (prepare(first_query), prepare(second_query))
    key_a = prepare(first_key).reshape(local_rows, head_count * head_width)
    key_b = prepare(second_key).reshape(local_rows, head_count * head_width)
    start_state = (
        jnp.full((local_rows, head_count), -1e30, jnp.float32),
        jnp.zeros((local_rows, head_count), jnp.float32),
        jnp.zeros((local_rows, head_count, value_width), jnp.float32),
    )
    piece_a = lax.all_gather(key_a, "sp", axis=0, tiled=True)
    piece_b = lax.all_gather(key_b, "sp", axis=0, tiled=True)
    piece_v = lax.all_gather(values, "sp", axis=0, tiled=True)
    count = piece_a.shape[0]
    block = 512
    blocks = count // block

    def advance(state, item):
        block_a, block_b, block_v = item
        return (
            (
                absorb(state[0], query_a, block_a, block_v, factor),
                absorb(state[1], query_b, block_b, block_v, factor),
            ),
            None,
        )

    items = (
        piece_a.reshape(blocks, block, head_count, head_width),
        piece_b.reshape(blocks, block, head_count, head_width),
        piece_v.reshape(blocks, block, head_count, value_width),
    )
    state_a, state_b = lax.scan(advance, (start_state, start_state), items)[0]
    diff = state_a[2] / state_a[1][..., None] - lambdas[None, :, None] * (
        state_b[2] / state_b[1][..., None]
    )
    scale = lax.rsqrt(jnp.mean(diff * diff, axis=-1, keepdims=True) + 1e-05)
    flat = (
        (diff * scale * head_gain * 0.8)
        .astype(jnp.bfloat16)
        .reshape(local_rows, head_count * value_width)
    )
    projected = lax.psum(
        jnp.dot(flat, out_weight, preferred_element_type=jnp.float32).astype(jnp.bfloat16), "tp"
    ).astype(jnp.float32)
    stream = lax.all_gather(residual, "tp", axis=0, tiled=True)
    whole = layer_norm(stream.astype(jnp.float32) + projected, norm_gain).astype(jnp.bfloat16)
    own_normed = lax.dynamic_slice_in_dim(
        whole, lax.axis_index("tp") * quarter_rows, quarter_rows, 0
    )
    lifted = jnp.dot(
        whole,
        lax.all_gather(up_weight, "sp", axis=0, tiled=True),
        preferred_element_type=jnp.float32,
    )
    down_full = lax.all_gather(down_weight, "sp", axis=1, tiled=True)
    hidden = jnp.square(jax.nn.relu(lifted)).astype(jnp.bfloat16)
    lowered = lax.psum_scatter(
        jnp.dot(hidden, down_full, preferred_element_type=jnp.float32).astype(jnp.bfloat16),
        "tp",
        scatter_dimension=0,
        tiled=True,
    ).astype(jnp.float32)
    return (own_normed.astype(jnp.float32) + lowered).astype(jnp.bfloat16)


BF = jnp.bfloat16
F32 = jnp.float32
VMEM_BUDGET = 40 * 2**20


def layer_kernel(
    n, nt, heads,
    qa_far, qb_far, ka_far, kb_far, v_far, inverse, lam, hgain, ow0, res0, ngain, up0, dn0,
    out,
    qm, kv0, kv, up, dn, ow, res, flat, normed, lifted, hidden, part, mine, got,
    top, total, summed, send, recv, load, qa, qb, ka, kb,
):
    s = lax.axis_index("sp")
    t = lax.axis_index("tp")
    rows, kv_width = kv0.shape
    width = qm.shape[2]
    value_width = (kv_width - 2 * width) // heads
    depth = up0.shape[0]
    units = up0.shape[1]
    model = ow0.shape[1]
    piece = res0.shape[0]
    mid = n // 2
    odd = s % 2
    place = (1 - odd) * (s // 2) + odd * (n - 1 - s // 2)

    def at_place(p):
        p = p % n
        hi = p // mid
        return (1 - hi) * (2 * p) + hi * (2 * (n - 1 - p) + 1)

    def owner(slot):
        return at_place(place - slot + n)

    right = {"sp": at_place(place + 1)}
    left = {"sp": at_place(place + n - 1)}
    mates = [{"tp": (t + d) % nt} for d in range(1, nt)]
    loads = [
        pltpu.make_async_copy(src, dst, load.at[i])
        for i, (src, dst) in enumerate(((up0, up.at[0]), (dn0, dn.at[0]), (ow0, ow.at[t])))
    ]
    entries = [
        pltpu.make_async_copy(src, dst, load.at[3 + i])
        for i, (src, dst) in enumerate((
            (ka_far, ka), (kb_far, kb), (v_far, kv0.at[:, pl.ds(2 * width, v_far.shape[1])]),
            (qa_far, qa), (qb_far, qb),
        ))
    ]
    for c in entries + loads:
        c.start()
    barrier = pltpu.get_barrier_semaphore()
    for peer in [right, left] + mates:
        pl.semaphore_signal(barrier, inc=1, device_id=peer, device_id_type=pl.DeviceIdType.MESH)
    pl.semaphore_wait(barrier, nt + 1)

    copies = []

    def remote(src, dst, peer):
        i = len(copies)
        c = pltpu.make_async_remote_copy(
            src_ref=src, dst_ref=dst, send_sem=send.at[i], recv_sem=recv.at[i],
            device_id=peer, device_id_type=pl.DeviceIdType.MESH,
        )
        c.start()
        copies.append(c)
        return c

    own_of = {"kv": (kv0, kv), "up": (up0, up), "dn": (dn0, dn)}
    groups = {}

    def issue(name, k, *which):
        own, buf = own_of[name]
        size = own.shape[0]
        for i in which:
            if k > 1:
                ready(name, k - 1, i)
            a = pl.ds(i * (size // 2), size // 2)
            b = pl.ds((1 - i) * (size // 2), size // 2)
            src_a = own.at[a] if k == 1 else buf.at[k - 1, a]
            src_b = own.at[b] if k == 1 else buf.at[n - k + 1, b]
            groups[name, k, i] = [
                remote(src_a, buf.at[k, a], right),
                remote(src_b, buf.at[n - k, b], left),
            ]

    def ready(name, k, *which):
        for i in which:
            arrive(groups[name, k, i])
            groups[name, k, i] = []

    def arrive(group):
        for c in group:
            c.wait_recv()

    def absorb(block):
        for which in range(2):
            keys = block[:, which * width : (which + 1) * width]
            for h in range(heads):
                at = which * heads + h
                scores = lax.dot_general(
                    keys, qm[which, h * rows : (h + 1) * rows, :],
                    (((1,), (1,)), ((), ())), preferred_element_type=F32,
                )
                old = top[at]
                peak = jnp.maximum(old, jnp.max(scores, axis=0, keepdims=True))
                shrink = jnp.exp(old - peak)
                e = jnp.exp(scores - peak)
                top[at] = peak
                total[at] = total[at] * shrink + jnp.sum(e, axis=0, keepdims=True)
                first = 2 * width + h * value_width
                vals = block[:, first : first + value_width]
                summed[at] = summed[at] * shrink + lax.dot_general(
                    vals, e.astype(BF), (((0,), (0,)), ((), ())), preferred_element_type=F32
                )

    def absorb_pair(k):
        def body(i, carry):
            absorb(kv[k + i * (n - 2 * k)])
            return carry

        lax.fori_loop(0, 2, body, 0)

    partner = {"tp": t + 1 - 2 * (t % 2)}
    issue("up", 1, 0)
    across = range(2, nt, 2)
    far = [
        (d, [remote(res0, res.at[t], {"tp": (t + d) % nt}), remote(ow0, ow.at[t], {"tp": (t + d) % nt})])
        for d in across
    ]
    near = [remote(res0, res.at[t], partner), remote(ow0, ow.at[t], partner)]
    head_width = width // heads
    half = head_width // 2
    lane = lax.broadcasted_iota(jnp.int32, (rows, width), 1)
    low = (lane % head_width) < half
    position = (lax.broadcasted_iota(jnp.int32, (rows, width), 0) + s * rows).astype(F32)
    angle = position * inverse[...]
    cos = jnp.cos(angle)
    sin = jnp.sin(angle)
    sin = jnp.where(low, -sin, sin)

    def turn(ref):
        x = ref[...].astype(F32)
        other = jnp.where(low, pltpu.roll(x, width - half, 1), pltpu.roll(x, half, 1))
        return x * cos + other * sin

    for c in entries:
        c.wait()
    kv0[:, :width] = turn(ka).astype(BF)
    kv0[:, width : 2 * width] = turn(kb).astype(BF)
    for which, ref in enumerate((qa, qb)):
        q = turn(ref).astype(BF).astype(F32) * head_width ** (-0.5)
        for h in range(heads):
            own = (lane // head_width) == h
            qm[which, h * rows : (h + 1) * rows, :] = jnp.where(own, q, 0.0).astype(BF)
    issue("kv", 1, 0, 1)
    issue("up", 1, 1)
    top[...] = jnp.full(top.shape, -1e30, F32)
    total[...] = jnp.zeros(total.shape, F32)
    summed[...] = jnp.zeros(summed.shape, F32)
    res[t] = res0[...]
    absorb(kv0[...])
    fillers = [("dn", 1, 0), ("dn", 1, 1), ("up", 2, 0, 1)]
    for k in range(1, mid):
        issue("kv", k + 1, 0)
        ready("kv", k, 1)
        if k + 1 < mid:
            issue("kv", k + 1, 1)
        if fillers:
            issue(*fillers.pop(0))
        absorb_pair(k)
    for filler in fillers:
        issue(*filler)
    ready("kv", mid, 0)
    issue("dn", 2, 0, 1)
    absorb(kv[mid])

    for h in range(heads):
        a = summed[h] / total[h]
        b = summed[heads + h] / total[heads + h]
        diff = a - lam[h] * b
        scale = lax.rsqrt(jnp.mean(diff * diff, axis=0, keepdims=True) + 1e-05)
        done = (diff * scale).T * hgain[...] * 0.8
        flat[0, :, h * value_width : (h + 1) * value_width] = done.astype(BF)

    got_flat = [remote(flat.at[0], flat.at[d + 1], m) for d, m in enumerate(mates)]
    for d, pair in far:
        arrive(pair)
        there = (t + nt - d) % nt
        near += [remote(res.at[there], res.at[there], partner), remote(ow.at[there], ow.at[there], partner)]
    arrive(near + got_flat)
    for c in loads:
        c.wait()

    chunk = piece
    def norm_rows(q, carry):
        rows_at = pl.ds(pl.multiple_of(q * chunk, chunk), chunk)
        stream = res[q].astype(F32) + jnp.dot(flat[0, rows_at, :], ow[t], preferred_element_type=F32)
        for d in range(1, nt):
            stream += jnp.dot(flat[d, rows_at, :], ow[(t + nt - d) % nt], preferred_element_type=F32)
        center = stream - jnp.mean(stream, axis=-1, keepdims=True)
        spread = jnp.mean(center * center, axis=-1, keepdims=True)
        row = (center * lax.rsqrt(spread + 1e-05) * ngain[...]).astype(BF)
        for i in range(n):
            normed[i, q] = row[:, i * depth : (i + 1) * depth]
        return carry

    lax.fori_loop(0, nt, norm_rows, 0)

    def lift(block, slot):
        x = normed[owner(slot)].reshape(rows, depth)
        return jnp.dot(x, block, preferred_element_type=F32)

    def lift_pair(k):
        def body(i, carry):
            slot = k + i * (n - 2 * k)
            lifted[...] += lift(up[slot], slot)
            return carry

        lax.fori_loop(0, 2, body, 0)

    lifted[...] = lift(up[0], 0)
    ready("up", 1, 0, 1)
    lift_pair(1)
    for k in range(2, mid):
        issue("up", k + 1, 0)
        if k + 1 < mid:
            issue("up", k + 1, 1)
        if k > 2:
            issue("dn", k, 0, 1)
        ready("up", k, 1)
        lift_pair(k)
    ready("up", mid, 0)
    h = jnp.maximum(lifted[...] + lift(up[mid], mid), 0.0)
    hidden[...] = (h * h).astype(BF)

    waits = []

    def lower(block, slot):
        y = jnp.dot(hidden[...], block, preferred_element_type=F32).reshape(nt, piece, depth)
        mine[slot] = y
        part[slot] = y.astype(BF)

    def share(slot):
        waits.append((slot, [
            remote(part.at[slot, (t + d) % nt], got.at[slot, d - 1], mates[d - 1])
            for d in range(1, nt)
        ]))

    def finish(slot, group):
        arrive(group)
        who = owner(slot)
        y = normed[who, t].astype(F32) + mine[slot, t]
        for d in range(nt - 1):
            y += got[slot, d].astype(F32)
        out[:, pl.ds(pl.multiple_of(who * depth, depth), depth)] = y.astype(BF)

    lower(dn[0], 0)
    ready("dn", 1, 0, 1)
    last = 0
    for k in range(1, mid):
        if k == mid - 1:
            issue("dn", mid, 0)
        ready("dn", k, 0, 1)
        for slot in (k, n - k):
            lower(dn[slot], slot)
            share(last)
            last = slot
    share(last)
    for slot, group in waits[:-2]:
        finish(slot, group)
    ready("dn", mid, 0)
    lower(dn[mid], mid)
    for slot, group in waits[-2:]:
        finish(slot, group)
    share(mid)
    finish(*waits[-1])
    for c in copies:
        c.wait_send()


def fused(n, nt, residual, first_query, second_query, first_key, second_key, values,
          lambdas, head_gain, out_weight, norm_gain, up_weight, down_weight):
    rows, width = first_query.shape
    heads = lambdas.shape[0]
    head_width = width // heads
    value_width = values.shape[1] // heads
    half = head_width // 2
    depth, units = up_weight.shape
    model = out_weight.shape[1]
    piece = residual.shape[0]
    inverse = 10000.0 ** (-np.arange(half) * 2.0 / head_width)
    inverse = np.tile(inverse, 2 * heads)[None, :].astype(np.float32)
    kv_width = 2 * width + heads * value_width
    vmem = pl.BlockSpec(memory_space=pltpu.VMEM)
    smem = pl.BlockSpec(memory_space=pltpu.SMEM)
    far = pl.BlockSpec(memory_space=pl.ANY)
    mid = n // 2
    count = 6 * (n - 1) + 3 * nt + (n + 1) * (nt - 1)
    maps = 2 * heads
    return pl.pallas_call(
        functools.partial(layer_kernel, n, nt, heads),
        out_shape=jax.ShapeDtypeStruct((piece, model), BF),
        in_specs=[far] * 5 + [vmem, smem, vmem, far, vmem, vmem, far, far],
        out_specs=vmem,
        scratch_shapes=[
            pltpu.VMEM((2, heads * rows, width), BF),
            pltpu.VMEM((rows, kv_width), BF),
            pltpu.VMEM((n, rows, kv_width), BF),
            pltpu.VMEM((n, depth, units), BF),
            pltpu.VMEM((n, units, depth), BF),
            pltpu.VMEM((nt,) + out_weight.shape, BF),
            pltpu.VMEM((nt, piece, model), BF),
            pltpu.VMEM((nt, rows, heads * value_width), BF),
            pltpu.VMEM((n, nt, piece, depth), BF),
            pltpu.VMEM((rows, units), F32),
            pltpu.VMEM((rows, units), BF),
            pltpu.VMEM((n, nt, piece, depth), BF),
            pltpu.VMEM((n, nt, piece, depth), F32),
            pltpu.VMEM((n, nt - 1, piece, depth), BF),
            pltpu.VMEM((maps, 1, rows), F32),
            pltpu.VMEM((maps, 1, rows), F32),
            pltpu.VMEM((maps, value_width, rows), F32),
            pltpu.SemaphoreType.DMA((count,)),
            pltpu.SemaphoreType.DMA((count,)),
            pltpu.SemaphoreType.DMA((8,)),
        ] + [pltpu.VMEM((rows, width), BF)] * 4,
        compiler_params=pltpu.CompilerParams(
            collective_id=0, has_side_effects=True, vmem_limit_bytes=60 * 2**20
        ),
        name="layer",
    )(first_query, second_query, first_key, second_key, values, inverse,
      lambdas, head_gain.reshape(1, -1), out_weight, residual,
      norm_gain.reshape(1, -1), up_weight, down_weight)


def choose(*args):
    n, nt = lax.axis_size("sp"), lax.axis_size("tp")
    gathered = n * sum(a.size * a.dtype.itemsize for a in (args[3], args[4], args[5], args[10], args[11]))
    gathered += nt * sum(a.size * a.dtype.itemsize for a in (args[0], args[8]))
    if n % 2 == 0 and n >= 6 and nt % 2 == 0 and 2 * gathered <= VMEM_BUDGET:
        return fused(n, nt, *args)
    return local(*args)


def solution(mesh):
    in_specs = (
        P(("sp", "tp"), None),
        P("sp", "tp"),
        P("sp", "tp"),
        P("sp", "tp"),
        P("sp", "tp"),
        P("sp", "tp"),
        P("tp"),
        P(),
        P("tp", None),
        P(),
        P("sp", "tp"),
        P("tp", "sp"),
    )
    out_specs = P(("sp", "tp"), None)
    return jax.shard_map(choose, mesh=mesh, in_specs=in_specs, out_specs=out_specs, check_vma=False)
```
